32 devices in a mesh: sp: 8 (over z, core), tp: 4 (over y, x).
Axes of the slice: x: 2, y: 2, z: 4, core: 2. Of those that a mesh axis runs over, the one named last changes fastest.
Arguments:
- b_gate: bfloat16 [2048, 1024], P('sp', 'tp'), may hold values from -6 to 6
- c_gate: bfloat16 [2048, 1024], P('sp', 'tp'), may hold values from -6 to 6
- h_in: bfloat16 [2048, 1024], P('sp', 'tp'), may hold values from -6 to 6
- docs: int32 [2048], replicated, may hold values from 0 to 3, never falling along the last dimension, each value on 1 to 1024 neighbouring positions
- conv_taps: bfloat16 [3, 1024], replicated, may hold values from -3 to 3
- out_weight: bfloat16 [1024, 4096], P(None, 'tp'), may hold values from -0.1875 to 0.1875
- residual_in: bfloat16 [2048, 4096], P('sp', 'tp'), may hold values from -52 to 52
- norm_gain: bfloat16 [4096], replicated, may hold values from 0.099609375 to 1.8984375
- expert_pick: int32 [2048, 2], P('sp'), may hold values from 0 to 7, as said below
- route_weight: float32 [2048, 2], P('sp'), may hold values from 0.5 to 2
- w_gate: bfloat16 [8, 4096, 2048], P('sp', None, 'tp'), may hold values from -0.09375 to 0.09375
- w_up: bfloat16 [8, 4096, 2048], P('sp', None, 'tp'), may hold values from -0.09375 to 0.09375
- w_down: bfloat16 [8, 2048, 4096], P('sp', None, 'tp'), may hold values from -0.125 to 0.125
Outputs:
- stream_out: bfloat16 [2048, 4096], P('sp', 'tp')
The draws below stay inside these ranges and needn't reach their ends.
Inputs may be any that keep to these rules, and one draw needn't show every extreme that they name: `expert_pick`: each row names 2 different experts of one group; group g holds experts g * 2 up to the next group's first.
All inputs are finite; a program needn't handle non-finite values.
Results may differ from the reference program's by a relative error of at most 0.012.
Values may be sent and summed in bfloat16 or wider, within the bound.
A program may use at most 64 MiB of HBM per device.

```python
import math
import jax
import jax.numpy as jnp
import numpy as np
from jax import lax

D = 4096
CH = 1024
FFE = 2048
GROUPS = 4
TOP_K = 2
TOK_DEV = 256
TOKENS = 2048
EXPERTS = 8
CAP = 80
N_SP = 8


def draw_expert_pick(key, part):
    per_group = EXPERTS // GROUPS
    key_group, key_first, key_second = jax.random.split(jax.random.fold_in(key, 11), 3)
    group_ids = jax.random.randint(key_group, (TOKENS,), 0, GROUPS)
    first_pick = jax.random.randint(key_first, (TOKENS,), 0, per_group)
    second_pick = (first_pick + jax.random.randint(key_second, (TOKENS,), 1, per_group)) % per_group
    return jnp.stack([group_ids * per_group + first_pick, group_ids * per_group + second_pick], axis=1).astype(jnp.int32)


def draw_residual_in(key, part):
    key_base, key_rows = jax.random.split(jax.random.fold_in(key, 23), 2)
    column_scale = jnp.exp(jnp.linspace(math.log(0.3), math.log(3.0), D)).astype(jnp.float32)
    row_scale = jnp.exp(jax.random.uniform(key_rows, (TOKENS, 1), jnp.float32, math.log(0.4), math.log(4.0)))
    base = jnp.clip(jax.random.normal(key_base, (TOKENS, D), jnp.float32), -4.0, 4.0)
    return (base * row_scale * column_scale[None, :]).astype(jnp.bfloat16)


def level_of(key, extent, cuts, low, largest):
    def one(axis_at, shards_of):
        draws = jax.random.uniform(jax.random.fold_in(jax.random.fold_in(key, 6), axis_at), (shards_of,), jnp.float32, low / len(cuts), largest / len(cuts))
        return jnp.repeat(jnp.exp(draws), extent[axis_at] // shards_of).reshape((-1,) + (1,) * (len(extent) - axis_at - 1))

    factor_of = one(*cuts[0])
    for cut in cuts[1:]:
        factor_of = factor_of * one(*cut)
    return factor_of


def profile(amount, total, reach, skew):
    weights = [(1 << 20) // math.isqrt(standing ** skew) + 1 for standing in range(2, amount + 1)]
    spare, counts = total - reach - (amount - 1), [1] * (amount - 1)
    while spare > 0:
        candidates = [i for i in range(amount - 1) if counts[i] < reach]
        mass, budget = sum([weights[i] for i in candidates]), spare
        for i in candidates:
            extra = min(reach - counts[i], max(1, budget * weights[i] // mass), spare)
            counts[i] = counts[i] + extra
            spare = spare - extra
    return np.array([reach] + counts)


def uneven_parts(rng, count, total, most, lean):
    if count == 2:
        one = jax.random.randint(rng, (), max(1, total - most), min(most, total - 1) + 1)
        return jnp.stack([one, total - one])
    sizes = jnp.asarray(profile(count, total, most, lean), jnp.int32)
    couples = (count - 1) // 2
    giver, sink = sizes[1:1 + 2 * couples:2], sizes[2:2 + 2 * couples:2]
    margin = jnp.minimum(giver - 1, most - sink)
    passed = jax.random.randint(jax.random.fold_in(rng, 1), (couples,), 0, 1 << 20) % (margin + 1)
    sizes = sizes.at[1:1 + 2 * couples:2].set(giver - passed).at[2:2 + 2 * couples:2].set(sink + passed)
    return sizes[jax.random.permutation(jax.random.fold_in(rng, 2), count)]


def normal_values(stream_key, dims, scale, most, cuts=(), held_as=jnp.bfloat16):
    loudness = level_of(stream_key, dims, cuts, -0.22, 0.18) if cuts else 1.0
    values = jax.random.normal(stream_key, dims, jnp.float32) * scale * loudness
    return jnp.minimum(jnp.maximum(values, -most), most).astype(held_as)


def setup_inputs(seed: int = 0) -> dict:
    splits = jax.random.split(jax.random.key(seed), 14)
    b_gate = normal_values(splits[0], (TOKENS, CH), 1.0, 6.0, ((0, 8), (1, 4)))
    c_gate = normal_values(splits[1], (TOKENS, CH), 1.0, 6.0, ((0, 8), (1, 4)))
    h_in = normal_values(splits[2], (TOKENS, CH), 1.0, 6.0, ((0, 8), (1, 4)))
    docs = jnp.searchsorted(jnp.cumsum(uneven_parts(splits[3], N_SP // 2, TOKENS, 4 * TOK_DEV, 1)), jnp.arange(TOKENS), side="right").astype(jnp.int32)
    conv_taps = normal_values(splits[4], (3, CH), 0.577, 3.0)
    out_weight = normal_values(splits[5], (CH, D), CH ** -0.5, 0.1875, ((1, 4),))
    residual_in = draw_residual_in(jax.random.fold_in(splits[13], 71), 0)
    norm_gain = jnp.clip(1.0 + 0.18 * jax.random.normal(splits[7], (D,), jnp.float32), 0.099609375, 1.8984375).astype(jnp.bfloat16)
    expert_pick = draw_expert_pick(jax.random.fold_in(splits[13], 71), 0)
    route_weight = jnp.clip(jnp.exp(math.log(2.0) - 1.3862944 * jax.random.uniform(splits[9], (TOKENS, TOP_K), jnp.float32) ** level_of(splits[9], (TOKENS, TOP_K), ((0, 8),), -0.2, 0.2)), 0.5, 2.0)
    w_gate = normal_values(splits[10], (EXPERTS, D, FFE), D ** -0.5, 0.09375, ((0, 8), (2, 4)))
    w_up = normal_values(splits[11], (EXPERTS, D, FFE), D ** -0.5, 0.09375, ((0, 8), (2, 4)))
    w_down = normal_values(splits[12], (EXPERTS, FFE, D), FFE ** -0.5, 0.125, ((0, 8), (2, 4)))
    return {"b_gate": b_gate, "c_gate": c_gate, "h_in": h_in, "docs": docs, "conv_taps": conv_taps, "out_weight": out_weight, "residual_in": residual_in, "norm_gain": norm_gain, "expert_pick": expert_pick, "route_weight": route_weight, "w_gate": w_gate, "w_up": w_up, "w_down": w_down}


NORM_EPS = 1e-06

def reference(b_gate, c_gate, h_in, docs, conv_taps, out_weight, residual_in, norm_gain, expert_pick, route_weight, w_gate, w_up, w_down):
    product = (c_gate.astype(jnp.float32) * h_in.astype(jnp.float32)).astype(jnp.bfloat16)
    product_f = product.astype(jnp.float32)
    tap_weights = conv_taps.astype(jnp.float32)
    conv_sum = tap_weights[0][None, :] * product_f
    for step_back in (1, 2):
        earlier = jnp.concatenate([jnp.zeros((step_back, CH), jnp.float32), product_f[:-step_back]], axis=0)
        earlier_doc = jnp.concatenate([jnp.full((step_back,), -1, jnp.int32), docs[:-step_back]], axis=0)
        same_doc = (earlier_doc == docs).astype(jnp.float32)[:, None]
        conv_sum = conv_sum + tap_weights[step_back][None, :] * earlier * same_doc
    conv_out = (b_gate.astype(jnp.float32) * conv_sum).astype(jnp.bfloat16)
    stream = (residual_in.astype(jnp.float32) + jnp.dot(conv_out, out_weight, preferred_element_type=jnp.float32)).astype(jnp.bfloat16)
    stream_f = stream.astype(jnp.float32)
    inverse = lax.rsqrt(lax.optimization_barrier(jnp.mean(stream_f * stream_f, axis=1, keepdims=True)) + NORM_EPS)
    normed = (stream_f * inverse * norm_gain.astype(jnp.float32)[None, :]).astype(jnp.bfloat16)
    per_block = expert_pick.reshape(N_SP, TOK_DEV * TOP_K)
    onehot = (per_block[:, :, None] == jnp.arange(EXPERTS, dtype=jnp.int32)[None, None, :]).astype(jnp.int32)
    slot_pos = lax.optimization_barrier(jnp.sum((jnp.cumsum(onehot, axis=1) - onehot) * onehot, axis=2))
    kept_mask = slot_pos < CAP
    block_ids = jnp.arange(N_SP, dtype=jnp.int32)[:, None]
    target = (per_block * N_SP + block_ids) * CAP + jnp.minimum(slot_pos, CAP - 1)
    target = jnp.where(kept_mask, target, EXPERTS * N_SP * CAP).astype(jnp.int32)
    assign_ids = jnp.arange(N_SP * TOK_DEV * TOP_K, dtype=jnp.int32).reshape(N_SP, TOK_DEV * TOP_K)
    table = jnp.full((EXPERTS * N_SP * CAP + 1,), -1, jnp.int32).at[target.reshape(-1)].set(assign_ids.reshape(-1))
    table = table[:-1].reshape(EXPERTS, N_SP * CAP)
    weights_flat = route_weight.reshape(-1)

    def one_expert(running, expert):
        sources = table[expert]
        filled = sources >= 0
        safe_ids = jnp.maximum(sources, 0)
        token_ids = safe_ids // TOP_K
        inputs = jnp.where(filled[:, None], normed[token_ids], jnp.zeros((), normed.dtype))
        gate_pre = jnp.dot(inputs, w_gate[expert], preferred_element_type=jnp.float32)
        up_pre = jnp.dot(inputs, w_up[expert], preferred_element_type=jnp.float32)
        hidden = (jax.nn.silu(gate_pre) * up_pre).astype(jnp.bfloat16)
        result = jnp.dot(hidden, w_down[expert], preferred_element_type=jnp.float32).astype(jnp.bfloat16)
        factor = jnp.where(filled, weights_flat[safe_ids], jnp.zeros((), weights_flat.dtype))
        scaled = result.astype(jnp.float32) * factor[:, None]
        return (running.at[token_ids].add(scaled), None)
    feed_out, unused = lax.scan(one_expert, jnp.zeros((TOKENS, D), jnp.float32), jnp.arange(EXPERTS, dtype=jnp.int32))
    return (stream_f + feed_out).astype(jnp.bfloat16)
```

```python
import functools

import jax
import jax.numpy as jnp
from jax import lax
from jax.experimental import pallas as pl
from jax.experimental.pallas import tpu as pltpu
from jax.sharding import PartitionSpec as P

TOP_K = 2
GROUPS = 4
MESH = pl.DeviceIdType.MESH


NORM_EPS = 1e-06


def passed_along(value, axis, steps):
    count = lax.axis_size(axis)
    first, last = (max(0, -steps), min(count, count - steps))
    return lax.ppermute(value, axis, [(source, source + steps) for source in range(first, last)])


def general(
    b_gate,
    c_gate,
    h_in,
    docs,
    conv_taps,
    out_weight,
    residual_in,
    norm_gain,
    expert_pick,
    route_weight,
    w_gate,
    w_up,
    w_down,
):
    tok_rows, local_chans = h_in.shape
    width = residual_in.shape[1]
    full_dim = w_gate.shape[1]
    n_sp = lax.axis_size("sp")
    sp_index = lax.axis_index("sp")
    tp_index = lax.axis_index("tp")
    first_pos = sp_index * tok_rows
    product = (c_gate.astype(jnp.float32) * h_in.astype(jnp.float32)).astype(jnp.bfloat16)
    edge = passed_along(product[tok_rows - 2 :], "sp", 1)
    extended = jnp.concatenate([edge, product], axis=0).astype(jnp.float32)
    own_docs = lax.dynamic_slice_in_dim(docs, first_pos, tok_rows)
    padded_docs = jnp.concatenate([jnp.full((2,), -1, jnp.int32), docs], axis=0)
    near_docs = lax.dynamic_slice_in_dim(padded_docs, first_pos, tok_rows + 2)
    tap_weights = lax.dynamic_slice_in_dim(
        conv_taps, tp_index * local_chans, local_chans, 1
    ).astype(jnp.float32)
    conv_sum = tap_weights[0][None, :] * extended[2:]
    for step_back in (1, 2):
        same_doc = (near_docs[2 - step_back : 2 - step_back + tok_rows] == own_docs).astype(
            jnp.float32
        )[:, None]
        conv_sum = (
            conv_sum
            + tap_weights[step_back][None, :]
            * extended[2 - step_back : 2 - step_back + tok_rows]
            * same_doc
        )
    conv_out = (b_gate.astype(jnp.float32) * conv_sum).astype(jnp.bfloat16)
    projected = jnp.dot(
        lax.all_gather(conv_out, "tp", axis=1, tiled=True),
        out_weight,
        preferred_element_type=jnp.float32,
    )
    stream = (residual_in.astype(jnp.float32) + projected).astype(jnp.bfloat16)
    stream_f = stream.astype(jnp.float32)
    capacity = 5 * tok_rows // (2 * n_sp)
    assign_flat = expert_pick.reshape(-1)
    onehot = (assign_flat[:, None] == jnp.arange(n_sp, dtype=jnp.int32)[None, :]).astype(jnp.int32)
    slot_pos = jnp.sum((jnp.cumsum(onehot, axis=0) - onehot) * onehot, axis=1)
    kept_mask = slot_pos < capacity
    target = jnp.where(
        kept_mask, assign_flat * capacity + jnp.minimum(slot_pos, capacity - 1), n_sp * capacity
    )
    table = (
        jnp.full((n_sp * capacity + 1,), -1, jnp.int32)
        .at[target]
        .set(jnp.arange(assign_flat.shape[0], dtype=jnp.int32))[:-1]
    )
    filled = table >= 0
    source_rows = jnp.maximum(table, 0) // TOP_K
    gate_local = w_gate[0]
    up_local = w_up[0]
    slot_rows = n_sp * capacity
    squares = lax.psum(jnp.sum(stream_f * stream_f, axis=1), "tp")
    inverse = lax.rsqrt(squares / full_dim + NORM_EPS)[:, None]
    gain_cols = lax.dynamic_slice_in_dim(norm_gain, tp_index * width, width).astype(jnp.float32)
    normed = (stream_f * inverse * gain_cols[None, :]).astype(jnp.bfloat16)
    outgoing = jnp.where(filled[:, None], normed[source_rows], jnp.zeros((), normed.dtype)).reshape(
        n_sp, capacity, width
    )
    received = lax.all_to_all(outgoing, "sp", split_axis=0, concat_axis=0, tiled=True)
    shard_piece = lax.all_gather(received, "tp", axis=2, tiled=True)
    flat_piece = shard_piece.reshape(slot_rows, shard_piece.shape[2])
    gate_pre = jnp.dot(flat_piece, gate_local, preferred_element_type=jnp.float32)
    up_pre = jnp.dot(flat_piece, up_local, preferred_element_type=jnp.float32)
    hidden = (jax.nn.silu(gate_pre) * up_pre).astype(jnp.bfloat16)
    down_local = w_down[0]
    result = jnp.dot(
        lax.all_gather(hidden, "tp", axis=1, tiled=True),
        down_local,
        preferred_element_type=jnp.float32,
    ).astype(jnp.bfloat16)
    returned = lax.all_to_all(
        result.reshape(n_sp, capacity, width), "sp", split_axis=0, concat_axis=0, tiled=True
    ).reshape(n_sp * capacity, width)
    picked = jnp.where(
        kept_mask[:, None],
        returned[jnp.minimum(target, n_sp * capacity - 1)].astype(jnp.float32),
        0.0,
    )
    weighted = picked * route_weight.reshape(-1)[:, None]
    feed_out = jnp.sum(weighted.reshape(tok_rows, TOP_K, width), axis=1)
    return (stream_f + feed_out).astype(jnp.bfloat16)


def flipped(index, mask):
    bit = 1
    while bit <= mask:
        if mask & bit:
            index = index + bit * (1 - 2 * ((index // bit) % 2))
        bit *= 2
    return index


def fused_kernel(
    n_chips,
    capacity,
    docs_ref,
    pick_ref,
    rw_ref,
    taps_ref,
    gain_ref,
    b_hbm,
    c_hbm,
    h_hbm,
    resid_hbm,
    ow_hbm,
    wg_hbm,
    wu_hbm,
    wd_hbm,
    out_ref,
    bb,
    cc,
    hh,
    resid,
    ow,
    wg,
    wu,
    wd,
    ext,
    cv,
    side,
    gain,
    stream,
    acc,
    pt,
    ptt,
    rows_out,
    wts_out,
    rows,
    wts,
    normed,
    hid,
    e_own,
    e_send,
    e_recv,
    feed_out,
    back,
    local_sems,
    send_sems,
    recv_sems,
):
    tok_rows, chans = hh.shape
    width = resid.shape[1]
    full = gain.shape[1]
    hid_cols = wg.shape[1]
    f32, bf16 = jnp.float32, jnp.bfloat16
    sp = lax.axis_index("sp")
    tp = lax.axis_index("tp")
    chip = sp // 2
    core = sp % 2
    tp_x = (tp // 2) * 2 + (1 - tp % 2)
    tp_y = (1 - tp // 2) * 2 + tp % 2
    tp_d = (1 - tp // 2) * 2 + (1 - tp % 2)
    dev_x = (sp, tp_x)
    dev_y = (sp, tp_y)
    dev_s = (chip * 2 + (1 - core), tp)
    ks = list(range(n_chips))
    dev_z = [(flipped(chip, k) * 2 + core, tp) for k in ks]

    barrier = pltpu.get_barrier_semaphore()
    peers = [dev_x, dev_y, dev_s] + dev_z[1:]
    for dev in peers:
        pl.semaphore_signal(barrier, inc=1, device_id=dev, device_id_type=MESH)
    other = jnp.where(core == 0, sp - 1, sp + 1)
    has_other = jnp.where(core == 0, chip > 0, chip < n_chips - 1)

    @pl.when(has_other)
    def _():
        pl.semaphore_signal(barrier, inc=1, device_id=(other, tp), device_id_type=MESH)

    pairs = (
        (c_hbm, cc), (h_hbm, hh), (b_hbm, bb), (resid_hbm, resid),
        (ow_hbm, ow), (wg_hbm.at[0], wg), (wu_hbm.at[0], wu), (wd_hbm.at[0], wd),
    )
    loads = [pltpu.make_async_copy(s, d, local_sems.at[i]) for i, (s, d) in enumerate(pairs)]
    for cp in loads:
        cp.start()

    count = [0]
    sent = []

    def remote(s, d, dev):
        i = count[0]
        count[0] += 1
        return pltpu.make_async_remote_copy(
            src_ref=s, dst_ref=d, send_sem=send_sems.at[i], recv_sem=recv_sems.at[i],
            device_id=dev, device_id_type=MESH,
        )

    def go(s, d, dev):
        cp = remote(s, d, dev)
        cp.start()
        sent.append(cp)
        return cp

    def cols(index, size):
        return pl.ds(pl.multiple_of(index * size, 128), size)

    sub8 = lax.broadcasted_iota(jnp.int32, (8, tok_rows), 0)
    own = docs_ref[:, cols(sp, tok_rows)]
    prev = docs_ref[:, pl.ds(pl.multiple_of(jnp.maximum(sp * tok_rows - 128, 0), 128), 128)]
    prev = jnp.where(sp > 0, prev, -1)
    near = jnp.broadcast_to(jnp.concatenate([prev, own], axis=1), (8, tok_rows + 128))
    own = jnp.broadcast_to(own, (8, tok_rows))
    same = [(pltpu.roll(near, lag, 1)[:, 128:] == own).astype(f32) for lag in (1, 2)]
    first = pick_ref[0:1, :]
    even = jnp.bitwise_and(first, 1) == 0
    w_a, w_b = rw_ref[0:1, :], rw_ref[1:2, :]
    table = [
        lax.shift_right_logical(first, 1).astype(f32),
        jnp.where(even, w_a, w_b),
        jnp.where(even, w_b, w_a),
    ]
    block = jnp.where(sub8 == 0, same[0], jnp.where(sub8 == 1, same[1], 0.0))
    for i, row in enumerate(table):
        block = jnp.where(sub8 == 2 + i, jnp.broadcast_to(row, (8, tok_rows)), block)
    block = jnp.concatenate([block, jnp.zeros((120, tok_rows), f32)], axis=0)
    side[...] = jnp.transpose(block)

    loads[0].wait()
    loads[1].wait()
    product = (cc[...].astype(f32) * hh[...].astype(f32)).astype(bf16)
    ext[8:, :] = product.astype(f32)
    with jax.named_scope("barrier"):
        pl.semaphore_wait(barrier, len(peers) + has_other.astype(jnp.int32))

    edge = remote(ext.at[pl.ds(tok_rows, 8)], ext.at[pl.ds(0, 8)], (sp + 1, tp))

    @pl.when(sp < 2 * n_chips - 1)
    def _():
        edge.start()

    loads[2].wait()

    @pl.when(sp > 0)
    def _():
        with jax.named_scope("edge"):
            edge.wait_recv()

    @pl.when(sp == 0)
    def _():
        ext[0:8, :] = jnp.zeros((8, chans), f32)

    taps = taps_ref[:, cols(tp, chans)].astype(f32)
    conv = taps[0:1, :] * ext[8 : 8 + tok_rows, :]
    for lag in (1, 2):
        conv = conv + taps[lag : lag + 1, :] * ext[8 - lag : 8 - lag + tok_rows, :] * side[:, lag - 1 : lag]
    cv[:, cols(tp, chans)] = (bb[...].astype(f32) * conv).astype(bf16)

    def put(buf, at, dev):
        part = buf.at[:, at]
        return go(part, part, dev)

    def spread_one(buf, size, g):
        half = size // 2
        g["xh"] = put(buf, cols(tp * 2 + 1, half), dev_x)
        g["yl"] = put(buf, cols(tp * 2, half), dev_y)

    def spread_two(buf, size, g):
        half = size // 2
        g["xl"] = put(buf, cols(tp * 2, half), dev_x)
        g["yh"] = put(buf, cols(tp * 2 + 1, half), dev_y)

    def relay(buf, size, g):
        half = size // 2
        g["yl"].wait_recv()
        g["dl"] = put(buf, cols(tp_y * 2, half), dev_x)
        g["xh"].wait_recv()
        g["dh"] = put(buf, cols(tp_x * 2 + 1, half), dev_y)

    cg = {}
    spread_one(cv, chans, cg)
    spread_two(cv, chans, cg)

    def proj(index):
        rows_ = pl.ds(pl.multiple_of(index * chans, 128), chans)
        return jnp.dot(cv[:, cols(index, chans)], ow[rows_, :], preferred_element_type=f32)

    loads[3].wait()
    loads[4].wait()
    acc[...] = resid[...].astype(f32) + proj(tp)

    lane = lax.broadcasted_iota(jnp.int32, (tok_rows, 128), 1)
    lane_f = lane.astype(f32)
    group = side[:, 2:3]
    onehot = (group == lane_f).astype(f32)
    earlier = (
        lax.broadcasted_iota(jnp.int32, (tok_rows, tok_rows), 1)
        < lax.broadcasted_iota(jnp.int32, (tok_rows, tok_rows), 0)
    ).astype(f32).astype(bf16)
    before = jnp.dot(earlier, onehot.astype(bf16), preferred_element_type=f32)
    slot = jnp.sum(before * onehot, axis=1, keepdims=True)

    def choose(k):
        here = flipped(chip, k).astype(f32)
        hit = jnp.where((group == here) & (slot == lane_f) & (lane < capacity), 1.0, 0.0)
        pt[k] = hit.astype(bf16)
        ptt[k * capacity : (k + 1) * capacity, :] = jnp.transpose(hit)[:capacity].astype(bf16)
        w0 = jnp.sum(hit * side[:, 3:4], axis=0, keepdims=True)
        w1 = jnp.sum(hit * side[:, 4:5], axis=0, keepdims=True)
        s8 = lax.broadcasted_iota(jnp.int32, (8, 128), 0)
        w0, w1 = jnp.broadcast_to(w0, (8, 128)), jnp.broadcast_to(w1, (8, 128))
        wts_out[k] = jnp.where(s8 == 0, w0, jnp.where(s8 == 1, w1, 0.0))

    choose(0)
    choose(1)
    with jax.named_scope("crelay"):
        relay(cv, chans, cg)
    for k in ks[2:]:
        choose(k)
    wts[0] = wts_out[0]
    gains = gain_ref[...].astype(f32)
    for j in range(full // 128):
        gain[:, j * 128 : (j + 1) * 128] = gains[j : j + 1, :]
    with jax.named_scope("cx"):
        cg["xl"].wait_recv()
    acc[...] += proj(tp_x)
    with jax.named_scope("cy"):
        cg["yh"].wait_recv()
    acc[...] += proj(tp_y)
    with jax.named_scope("cd"):
        cg["dl"].wait_recv()
        cg["dh"].wait_recv()
    stream[...] = (acc[...] + proj(tp_d)).astype(bf16)

    mine = cols(tp, width)
    rg, hg = [{} for _ in ks], [{} for _ in ks]
    sis = [[] for _ in ks]
    z_rows, z_wts, e_sends, z_back = [[None] * n_chips for _ in range(4)]

    def share(k, index, size):
        at = cols(index, size)
        sis[k].append(go(rows.at[k, 0, :, at], rows.at[k, 1, :, at], dev_s))

    def select(k):
        at = slice(k * capacity, (k + 1) * capacity)
        return jnp.dot(ptt[at, :], stream[...], preferred_element_type=f32).astype(bf16)

    def rows_send(k):
        if k == 0:
            rows[0, 0, :, mine] = select(0)
        else:
            z_rows[k].wait_recv()
        spread_one(rows.at[k, 0], width, rg[k])
        spread_two(rows.at[k, 0], width, rg[k])
        share(k, tp, width)

    def z_send(k):
        rows_out[k] = select(k)
        z_rows[k] = go(rows_out.at[k], rows.at[k, 0, :, mine], dev_z[k])
        z_wts[k] = go(wts_out.at[k], wts.at[k], dev_z[k])

    def rows_relay(k):
        relay(rows.at[k, 0], width, rg[k])

    def rows_near(k):
        rg[k]["xl"].wait_recv()
        share(k, tp_x, width)
        rg[k]["yh"].wait_recv()
        share(k, tp_y, width)

    def rows_far(k):
        rg[k]["dl"].wait_recv()
        share(k, tp_d * 2, width // 2)
        rg[k]["dh"].wait_recv()
        share(k, tp_d * 2 + 1, width // 2)

    def norm(k, p):
        if p == 1:
            for cp in sis[k]:
                cp.wait_recv()

        def body(r, carry):
            at = pl.ds(pl.multiple_of(r * 16, 16), 16)
            x = rows[k, p, at, :].astype(f32)
            ms = jnp.sum(x * x, axis=1, keepdims=True) / full
            inv = lax.rsqrt(ms + NORM_EPS)
            y = (x * inv * gain[...]).astype(bf16)
            normed[pl.ds(pl.multiple_of(p * capacity + r * 16, 16), 16), :] = y
            return carry

        lax.fori_loop(0, capacity // 16, body, 0)

    def up(k):
        if k == 0:
            loads[5].wait()
            loads[6].wait()

        def tile(n, carry):
            at = pl.ds(pl.multiple_of(n * 256, 256), 256)
            x = normed[...]
            g = jnp.dot(x, wg[:, at], preferred_element_type=f32)
            u = jnp.dot(x, wu[:, at], preferred_element_type=f32)
            h = (g / (1.0 + jnp.exp(-g)) * u).astype(bf16)
            hid[k, :, pl.ds(pl.multiple_of(tp * hid_cols + n * 256, 256), 256)] = h
            return carry

        lax.fori_loop(0, hid_cols // 256, tile, 0)

    def hid_one(k):
        spread_one(hid.at[k], hid_cols, hg[k])

    def hid_two(k):
        spread_two(hid.at[k], hid_cols, hg[k])

    def hid_relay(k):
        relay(hid.at[k], hid_cols, hg[k])

    waited = []

    def down(k):
        for name in ("xl", "yh", "dl", "dh"):
            hg[k][name].wait_recv()
        if not waited:
            loads[7].wait()
            waited.append(k)

        def tile(n, carry):
            at = pl.ds(pl.multiple_of(n * 256, 256), 256)
            e = jnp.dot(hid[k], wd[:, at], preferred_element_type=f32).astype(bf16)
            e_own[k, :, at] = e[:capacity]
            e_send[k, :, at] = e[capacity:]
            return carry

        lax.fori_loop(0, width // 256, tile, 0)
        e_sends[k] = go(e_send.at[k], e_recv.at[k], dev_s)

    def column(row):
        l128 = lax.broadcasted_iota(jnp.int32, (capacity, 128), 1)
        s128 = lax.broadcasted_iota(jnp.int32, (capacity, 128), 0)
        return jnp.sum(jnp.where(l128 == s128, row, 0.0), axis=1, keepdims=True)

    def combine(k):
        if k > 0:
            z_wts[k].wait_recv()
        w = wts[k]
        w_even, w_odd = column(w[0:1, :]), column(w[1:2, :])
        pick = core.astype(f32)
        w_mine = w_even * (1.0 - pick) + w_odd * pick
        w_other = w_odd * (1.0 - pick) + w_even * pick
        e_sends[k].wait_recv()
        f = (e_own[k].astype(f32) * w_mine + e_recv[k].astype(f32) * w_other).astype(bf16)
        if k == 0:
            back[0, 0:capacity, :] = f
        else:
            feed_out[k] = f
            z_back[k] = go(feed_out.at[k], back.at[k, pl.ds(0, capacity), :], dev_z[k])

    def gather(k):
        if k > 0:
            z_back[k].wait_recv()
        got = jnp.dot(pt[k], back[k], preferred_element_type=f32)
        if k == 0:
            out_ref[...] = (acc[...] + got).astype(bf16)
        else:
            acc[...] += got

    def clear():
        acc[...] = stream[...].astype(f32)
        for k in ks:
            back[k, capacity:, :] = jnp.zeros((128 - capacity, width), bf16)

    def near_far(k):
        rows_near(k)
        rows_far(k)

    plan = [
        (rows_send, 0), (z_send, 1), (clear,), (rows_relay, 0), (z_send, 2), (rows_near, 0), (rows_send, 1),
        (rows_far, 0), (z_send, 3), (norm, 0, 0), (rows_relay, 1), (norm, 0, 1), (up, 0), (rows_send, 2),
        (near_far, 1), (norm, 1, 0), (rows_relay, 2), (norm, 1, 1), (up, 1), (rows_send, 3), (near_far, 2),
        (norm, 2, 0), (rows_relay, 3), (norm, 2, 1), (up, 2), (hid_one, 2), (hid_two, 2), (hid_one, 0),
        (near_far, 3), (norm, 3, 0), (hid_relay, 2), (norm, 3, 1), (up, 3), (hid_one, 3), (hid_two, 3),
        (hid_one, 1), (down, 2), (hid_relay, 3), (hid_two, 1), (combine, 2), (hid_relay, 1), (hid_two, 0),
        (hid_relay, 0), (down, 3), (combine, 3), (down, 1), (combine, 1), (gather, 2), (down, 0), (combine, 0),
        (gather, 3), (gather, 1), (gather, 0),
    ]

    for step, *args in plan:
        name = step.__name__ + "".join("_" + str(a) for a in args)
        with jax.named_scope(name):
            step(*args)

    with jax.named_scope("drain"):
        for cp in sent:
            cp.wait_send()

        @pl.when(sp < 2 * n_chips - 1)
        def _():
            edge.wait_send()


def fused(
    b_gate,
    c_gate,
    h_in,
    docs,
    conv_taps,
    out_weight,
    residual_in,
    norm_gain,
    expert_pick,
    route_weight,
    w_gate,
    w_up,
    w_down,
):
    tok_rows, chans = h_in.shape
    width = residual_in.shape[1]
    full = w_gate.shape[1]
    hid_full = w_down.shape[1]
    n_sp = lax.axis_size("sp")
    n_chips = n_sp // 2
    capacity = 5 * tok_rows // (2 * n_sp)
    n_copies = 7 + 18 * n_chips + 3 * (n_chips - 1)
    vmem = pl.BlockSpec(memory_space=pltpu.VMEM)
    hbm = pl.BlockSpec(memory_space=pltpu.HBM)
    bf16, f32 = jnp.bfloat16, jnp.float32
    return pl.pallas_call(
        functools.partial(fused_kernel, n_chips, capacity),
        out_shape=pltpu.VMEM((tok_rows, width), bf16),
        in_specs=[vmem] * 5 + [hbm] * 8,
        out_specs=vmem,
        scratch_shapes=[
            pltpu.VMEM(b_gate.shape, bf16),
            pltpu.VMEM(c_gate.shape, bf16),
            pltpu.VMEM(h_in.shape, bf16),
            pltpu.VMEM(residual_in.shape, bf16),
            pltpu.VMEM(out_weight.shape, bf16),
            pltpu.VMEM(w_gate.shape[1:], bf16),
            pltpu.VMEM(w_up.shape[1:], bf16),
            pltpu.VMEM(w_down.shape[1:], bf16),
            pltpu.VMEM((tok_rows + 8, chans), f32),
            pltpu.VMEM((tok_rows, out_weight.shape[0]), bf16),
            pltpu.VMEM((tok_rows, 128), f32),
            pltpu.VMEM((1, full), f32),
            pltpu.VMEM((tok_rows, width), bf16),
            pltpu.VMEM((tok_rows, width), f32),
            pltpu.VMEM((n_chips, tok_rows, 128), bf16),
            pltpu.VMEM((n_chips * capacity, tok_rows), bf16),
            pltpu.VMEM((n_chips, capacity, width), bf16),
            pltpu.VMEM((n_chips, 8, 128), f32),
            pltpu.VMEM((n_chips, 2, capacity, full), bf16),
            pltpu.VMEM((n_chips, 8, 128), f32),
            pltpu.VMEM((2 * capacity, full), bf16),
            pltpu.VMEM((n_chips, 2 * capacity, hid_full), bf16),
            pltpu.VMEM((n_chips, capacity, width), bf16),
            pltpu.VMEM((n_chips, capacity, width), bf16),
            pltpu.VMEM((n_chips, capacity, width), bf16),
            pltpu.VMEM((n_chips, capacity, width), bf16),
            pltpu.VMEM((n_chips, 128, width), bf16),
            pltpu.SemaphoreType.DMA((8,)),
            pltpu.SemaphoreType.DMA((n_copies,)),
            pltpu.SemaphoreType.DMA((n_copies,)),
        ],
        compiler_params=pltpu.CompilerParams(
            collective_id=0, has_side_effects=True, vmem_limit_bytes=66519040
        ),
    )(
        docs.reshape(1, -1),
        expert_pick.T,
        route_weight.T,
        conv_taps,
        norm_gain.reshape(-1, 128),
        b_gate,
        c_gate,
        h_in,
        residual_in,
        out_weight,
        w_gate,
        w_up,
        w_down,
    )


def pairs_fit(mesh):
    n_sp, n_tp = mesh.shape["sp"], mesh.shape["tp"]
    return n_sp == GROUPS * TOP_K and TOP_K == 2 and n_tp == 4


def solution(mesh):
    return jax.shard_map(
        fused if pairs_fit(mesh) else general,
        mesh=mesh,
        in_specs=(
            P("sp", "tp"),
            P("sp", "tp"),
            P("sp", "tp"),
            P(),
            P(),
            P(None, "tp"),
            P("sp", "tp"),
            P(),
            P("sp", None),
            P("sp", None),
            P("sp", None, "tp"),
            P("sp", None, "tp"),
            P("sp", None, "tp"),
        ),
        out_specs=P("sp", "tp"),
        check_vma=False,
    )
```

```python
import functools

import jax
import jax.numpy as jnp
from jax import lax
from jax.experimental import pallas as pl
from jax.experimental.pallas import tpu as pltpu
from jax.sharding import PartitionSpec as P

TOP_K = 2
GROUPS = 4
MESH = pl.DeviceIdType.MESH


NORM_EPS = 1e-06


def passed_along(value, axis, steps):
    count = lax.axis_size(axis)
    first, last = (max(0, -steps), min(count, count - steps))
    return lax.ppermute(value, axis, [(source, source + steps) for source in range(first, last)])


def general(
    b_gate,
    c_gate,
    h_in,
    docs,
    conv_taps,
    out_weight,
    residual_in,
    norm_gain,
    expert_pick,
    route_weight,
    w_gate,
    w_up,
    w_down,
):
    tok_rows, local_chans = h_in.shape
    width = residual_in.shape[1]
    full_dim = w_gate.shape[1]
    n_sp = lax.axis_size("sp")
    sp_index = lax.axis_index("sp")
    tp_index = lax.axis_index("tp")
    first_pos = sp_index * tok_rows
    product = (c_gate.astype(jnp.float32) * h_in.astype(jnp.float32)).astype(jnp.bfloat16)
    edge = passed_along(product[tok_rows - 2 :], "sp", 1)
    extended = jnp.concatenate([edge, product], axis=0).astype(jnp.float32)
    own_docs = lax.dynamic_slice_in_dim(docs, first_pos, tok_rows)
    padded_docs = jnp.concatenate([jnp.full((2,), -1, jnp.int32), docs], axis=0)
    near_docs = lax.dynamic_slice_in_dim(padded_docs, first_pos, tok_rows + 2)
    tap_weights = lax.dynamic_slice_in_dim(
        conv_taps, tp_index * local_chans, local_chans, 1
    ).astype(jnp.float32)
    conv_sum = tap_weights[0][None, :] * extended[2:]
    for step_back in (1, 2):
        same_doc = (near_docs[2 - step_back : 2 - step_back + tok_rows] == own_docs).astype(
            jnp.float32
        )[:, None]
        conv_sum = (
            conv_sum
            + tap_weights[step_back][None, :]
            * extended[2 - step_back : 2 - step_back + tok_rows]
            * same_doc
        )
    conv_out = (b_gate.astype(jnp.float32) * conv_sum).astype(jnp.bfloat16)
    projected = jnp.dot(
        lax.all_gather(conv_out, "tp", axis=1, tiled=True),
        out_weight,
        preferred_element_type=jnp.float32,
    )
    stream = (residual_in.astype(jnp.float32) + projected).astype(jnp.bfloat16)
    stream_f = stream.astype(jnp.float32)
    capacity = 5 * tok_rows // (2 * n_sp)
    assign_flat = expert_pick.reshape(-1)
    onehot = (assign_flat[:, None] == jnp.arange(n_sp, dtype=jnp.int32)[None, :]).astype(jnp.int32)
    slot_pos = jnp.sum((jnp.cumsum(onehot, axis=0) - onehot) * onehot, axis=1)
    kept_mask = slot_pos < capacity
    target = jnp.where(
        kept_mask, assign_flat * capacity + jnp.minimum(slot_pos, capacity - 1), n_sp * capacity
    )
    table = (
        jnp.full((n_sp * capacity + 1,), -1, jnp.int32)
        .at[target]
        .set(jnp.arange(assign_flat.shape[0], dtype=jnp.int32))[:-1]
    )
    filled = table >= 0
    source_rows = jnp.maximum(table, 0) // TOP_K
    gate_local = w_gate[0]
    up_local = w_up[0]
    slot_rows = n_sp * capacity
    squares = lax.psum(jnp.sum(stream_f * stream_f, axis=1), "tp")
    inverse = lax.rsqrt(squares / full_dim + NORM_EPS)[:, None]
    gain_cols = lax.dynamic_slice_in_dim(norm_gain, tp_index * width, width).astype(jnp.float32)
    normed = (stream_f * inverse * gain_cols[None, :]).astype(jnp.bfloat16)
    outgoing = jnp.where(filled[:, None], normed[source_rows], jnp.zeros((), normed.dtype)).reshape(
        n_sp, capacity, width
    )
    received = lax.all_to_all(outgoing, "sp", split_axis=0, concat_axis=0, tiled=True)
    shard_piece = lax.all_gather(received, "tp", axis=2, tiled=True)
    flat_piece = shard_piece.reshape(slot_rows, shard_piece.shape[2])
    gate_pre = jnp.dot(flat_piece, gate_local, preferred_element_type=jnp.float32)
    up_pre = jnp.dot(flat_piece, up_local, preferred_element_type=jnp.float32)
    hidden = (jax.nn.silu(gate_pre) * up_pre).astype(jnp.bfloat16)
    down_local = w_down[0]
    result = jnp.dot(
        lax.all_gather(hidden, "tp", axis=1, tiled=True),
        down_local,
        preferred_element_type=jnp.float32,
    ).astype(jnp.bfloat16)
    returned = lax.all_to_all(
        result.reshape(n_sp, capacity, width), "sp", split_axis=0, concat_axis=0, tiled=True
    ).reshape(n_sp * capacity, width)
    picked = jnp.where(
        kept_mask[:, None],
        returned[jnp.minimum(target, n_sp * capacity - 1)].astype(jnp.float32),
        0.0,
    )
    weighted = picked * route_weight.reshape(-1)[:, None]
    feed_out = jnp.sum(weighted.reshape(tok_rows, TOP_K, width), axis=1)
    return (stream_f + feed_out).astype(jnp.bfloat16)


def flipped(index, mask):
    bit = 1
    while bit <= mask:
        if mask & bit:
            index = index + bit * (1 - 2 * ((index // bit) % 2))
        bit *= 2
    return index


def fused_kernel(
    n_chips,
    capacity,
    docs_ref,
    pick_ref,
    rw_ref,
    taps_ref,
    gain_ref,
    b_hbm,
    c_hbm,
    h_hbm,
    resid_hbm,
    ow_hbm,
    wg_hbm,
    wu_hbm,
    wd_hbm,
    out_ref,
    bb,
    cc,
    hh,
    resid,
    ow,
    wg,
    wu,
    wd,
    ext,
    cv,
    side,
    gain,
    stream,
    acc,
    pt,
    ptt,
    rows_out,
    wts_out,
    rows,
    wts,
    normed,
    hid,
    e_own,
    e_send,
    e_recv,
    feed_out,
    back,
    up_sems,
    local_sems,
    send_sems,
    recv_sems,
):
    tok_rows, chans = hh.shape
    width = resid.shape[1]
    full = gain.shape[1]
    hid_cols = wg.shape[1]
    f32, bf16 = jnp.float32, jnp.bfloat16
    sp = lax.axis_index("sp")
    tp = lax.axis_index("tp")
    chip = sp // 2
    core = sp % 2
    tp_x = (tp // 2) * 2 + (1 - tp % 2)
    tp_y = (1 - tp // 2) * 2 + tp % 2
    tp_d = (1 - tp // 2) * 2 + (1 - tp % 2)
    dev_x = (sp, tp_x)
    dev_y = (sp, tp_y)
    dev_d = (sp, tp_d)
    dev_s = (chip * 2 + (1 - core), tp)
    ks = list(range(n_chips))
    dev_z = [(flipped(chip, k) * 2 + core, tp) for k in ks]

    barrier = pltpu.get_barrier_semaphore()
    plane = [dev_x, dev_y, dev_d, dev_s]
    above = [flipped(chip, k) > chip for k in ks]
    edge_down = (core == 0) & (chip > 0)
    edge_up = (core == 1) & (chip < n_chips - 1)

    def signal(sem, dev):
        pl.semaphore_signal(sem, inc=1, device_id=dev, device_id_type=MESH)

    for dev in plane:
        signal(barrier, dev)
    for k in ks[1:]:
        pl.when(above[k])(functools.partial(signal, barrier, dev_z[k]))
    pl.when(edge_up)(functools.partial(signal, barrier, (sp + 1, tp)))

    pairs = (
        (c_hbm, cc), (h_hbm, hh), (b_hbm, bb), (resid_hbm, resid),
        (ow_hbm, ow), (wg_hbm.at[0], wg), (wu_hbm.at[0], wu), (wd_hbm.at[0], wd),
    )
    loads = [pltpu.make_async_copy(s, d, local_sems.at[i]) for i, (s, d) in enumerate(pairs)]
    for cp in loads:
        cp.start()

    count = [2, 0]
    room = [rows.size * 2, hid.size * 2]
    sent = []

    def recv_sem():
        count[1] += 1
        return recv_sems.at[count[1] - 1]

    def remote(s, d, dev, recv=None, own_send=False):
        size = s.size * jnp.dtype(s.dtype).itemsize
        fits = [i for i in (0, 1) if room[i] >= size and size % (capacity * width) == 0]
        if fits:
            i = fits[0]
            room[i] -= size
        else:
            i = count[0]
            count[0] += 1
        cp = pltpu.make_async_remote_copy(
            src_ref=s, dst_ref=d, send_sem=send_sems.at[i],
            recv_sem=recv_sem() if recv is None else recv,
            device_id=dev, device_id_type=MESH,
        )
        if not fits and not own_send:
            sent.append(cp)
        return cp

    def go(s, d, dev, recv=None, own_send=False):
        cp = remote(s, d, dev, recv, own_send)
        cp.start()
        return cp

    def await_bytes(ref, recv):
        pltpu.make_async_remote_copy(
            src_ref=ref, dst_ref=ref, send_sem=send_sems.at[0], recv_sem=recv,
            device_id=dev_x, device_id_type=MESH,
        ).wait_recv()

    def cols(index, size):
        return pl.ds(pl.multiple_of(index * size, 128), size)

    sub8 = lax.broadcasted_iota(jnp.int32, (8, tok_rows), 0)
    own = docs_ref[:, cols(sp, tok_rows)]
    prev = docs_ref[:, pl.ds(pl.multiple_of(jnp.maximum(sp * tok_rows - 128, 0), 128), 128)]
    prev = jnp.where(sp > 0, prev, -1)
    near = jnp.broadcast_to(jnp.concatenate([prev, own], axis=1), (8, tok_rows + 128))
    own = jnp.broadcast_to(own, (8, tok_rows))
    same = [(pltpu.roll(near, lag, 1)[:, 128:] == own).astype(f32) for lag in (1, 2)]
    first = pick_ref[0:1, :]
    even = jnp.bitwise_and(first, 1) == 0
    w_a, w_b = rw_ref[0:1, :], rw_ref[1:2, :]
    table = [
        lax.shift_right_logical(first, 1).astype(f32),
        jnp.where(even, w_a, w_b),
        jnp.where(even, w_b, w_a),
    ]
    block = jnp.where(sub8 == 0, same[0], jnp.where(sub8 == 1, same[1], 0.0))
    for i, row in enumerate(table):
        block = jnp.where(sub8 == 2 + i, jnp.broadcast_to(row, (8, tok_rows)), block)
    block = jnp.concatenate([block, jnp.zeros((120, tok_rows), f32)], axis=0)
    side[...] = jnp.transpose(block)

    loads[0].wait()
    loads[1].wait()
    product = (cc[...].astype(f32) * hh[...].astype(f32)).astype(bf16)
    ext[8:, :] = product.astype(f32)
    with jax.named_scope("barrier"):
        pl.semaphore_wait(barrier, len(plane) + chip + edge_down.astype(jnp.int32))
    for k in ks[1:]:
        pl.when(flipped(chip, k) < chip)(functools.partial(signal, up_sems.at[k], dev_z[k]))
    pl.when(edge_down)(functools.partial(signal, up_sems.at[0], (sp - 1, tp)))

    edge = remote(ext.at[pl.ds(tok_rows, 8)], ext.at[pl.ds(0, 8)], (sp + 1, tp), None, True)
    pl.when(core == 0)(edge.start)
    loads[2].wait()
    taps = taps_ref[:, cols(tp, chans)].astype(f32)

    def conv(lo, hi):
        total = taps[0:1, :] * ext[8 + lo : 8 + hi, :]
        for lag in (1, 2):
            part = ext[8 + lo - lag : 8 + hi - lag, :]
            total = total + taps[lag : lag + 1, :] * part * side[lo:hi, lag - 1 : lag]
        cv[lo:hi, cols(tp, chans)] = (bb[lo:hi, :].astype(f32) * total).astype(bf16)

    head = 16
    conv(head, tok_rows)

    def put(buf, at, dev, recv=None, own_send=False):
        part = buf.at[:, at]
        return go(part, part, dev, recv, own_send)

    def send_yl(buf, size, g):
        g["yl"] = put(buf, cols(tp * 2, size // 2), dev_y)

    def send_xh(buf, size, g):
        g["xh"] = put(buf, cols(tp * 2 + 1, size // 2), dev_x)

    def send_xl(buf, size, g):
        put(buf, cols(tp * 2, size // 2), dev_x, g["late"])

    def send_yh(buf, size, g):
        put(buf, cols(tp * 2 + 1, size // 2), dev_y, g["late"])

    def spread(buf, size, g):
        g["late"] = recv_sem()
        for send in (send_yl, send_xh, send_xl, send_yh):
            send(buf, size, g)

    def relay_x(buf, size, g):
        g["yl"].wait_recv()
        if "far" not in g:
            g["far"] = recv_sem()
        put(buf, cols(tp_y * 2, size // 2), dev_x, g["far"])

    def relay_y(buf, size, g):
        g["xh"].wait_recv()
        if "far" not in g:
            g["far"] = recv_sem()
        put(buf, cols(tp_x * 2 + 1, size // 2), dev_y, g["far"])

    def relay(buf, size, g):
        relay_x(buf, size, g)
        relay_y(buf, size, g)

    cg = {}
    body = cv.at[pl.ds(head, tok_rows - head)]
    spread(body, chans, cg)

    def proj(index):
        rows_ = pl.ds(pl.multiple_of(index * chans, 128), chans)
        return jnp.dot(cv[:, cols(index, chans)], ow[rows_, :], preferred_element_type=f32)

    @pl.when(edge_up)
    def _():
        pl.semaphore_wait(up_sems.at[0], 1)
        edge.start()


    lane = lax.broadcasted_iota(jnp.int32, (tok_rows, 128), 1)
    lane_f = lane.astype(f32)
    group = side[:, 2:3]
    onehot = (group == lane_f).astype(f32)
    earlier = (
        lax.broadcasted_iota(jnp.int32, (tok_rows, tok_rows), 1)
        < lax.broadcasted_iota(jnp.int32, (tok_rows, tok_rows), 0)
    ).astype(f32).astype(bf16)
    before = jnp.dot(earlier, onehot.astype(bf16), preferred_element_type=f32)
    slot = jnp.sum(before * onehot, axis=1, keepdims=True)

    def choose(k):
        here = flipped(chip, k).astype(f32)
        hit = jnp.where((group == here) & (slot == lane_f) & (lane < capacity), 1.0, 0.0)
        pt[k] = hit.astype(bf16)
        ptt[k * capacity : (k + 1) * capacity, :] = jnp.transpose(hit)[:capacity].astype(bf16)
        w0 = jnp.sum(hit * side[:, 3:4], axis=0, keepdims=True)
        w1 = jnp.sum(hit * side[:, 4:5], axis=0, keepdims=True)
        s8 = lax.broadcasted_iota(jnp.int32, (8, 128), 0)
        w0, w1 = jnp.broadcast_to(w0, (8, 128)), jnp.broadcast_to(w1, (8, 128))
        wts_out[k] = jnp.where(s8 == 0, w0, jnp.where(s8 == 1, w1, 0.0))

    choose(0)

    @pl.when(sp > 0)
    def _():
        with jax.named_scope("edge"):
            edge.wait_recv()

    @pl.when(sp == 0)
    def _():
        ext[0:8, :] = jnp.zeros((8, chans), f32)

    conv(0, head)
    top, top_sem = cv.at[pl.ds(0, head), cols(tp, chans)], recv_sem()
    for dev in (dev_x, dev_y, dev_d):
        go(top, top, dev, top_sem)
    loads[3].wait()
    loads[4].wait()
    acc[...] = resid[...].astype(f32) + proj(tp)
    with jax.named_scope("crelay"):
        relay(body, chans, cg)
    for k in ks[1:]:
        choose(k)
    wts[0] = wts_out[0]
    gains = gain_ref[...].astype(f32)
    for j in range(full // 128):
        gain[:, j * 128 : (j + 1) * 128] = gains[j : j + 1, :]
    with jax.named_scope("top"):
        await_bytes(cv.at[pl.ds(0, head), pl.ds(0, 3 * chans)], top_sem)
    with jax.named_scope("cx"):
        await_bytes(body.at[:, pl.ds(0, chans)], cg["late"])
    acc[...] += proj(tp_x)
    acc[...] += proj(tp_y)
    with jax.named_scope("cd"):
        await_bytes(body.at[:, pl.ds(0, chans)], cg["far"])
    stream[...] = (acc[...] + proj(tp_d)).astype(bf16)

    mine = cols(tp, width)
    rg, hg = [{} for _ in ks], [{} for _ in ks]
    sis = [recv_sem() for _ in ks]
    z_rows, z_wts = [None] * n_chips, [None] * n_chips

    def share(k, index, size):
        at = cols(index, size)
        go(rows.at[k, 0, :, at], rows.at[k, 1, :, at], dev_s, sis[k])

    def select(k):
        at = slice(k * capacity, (k + 1) * capacity)
        return jnp.dot(ptt[at, :], stream[...], preferred_element_type=f32).astype(bf16)

    def rows_send(k):
        if k == 0:
            rows[0, 0, :, mine] = select(0)
        else:
            z_rows[k].wait_recv()
        spread(rows.at[k, 0], width, rg[k])
        share(k, tp, width)

    def z_pick(k):
        rows_out[k] = select(k)
        z_rows[k] = remote(rows_out.at[k], rows.at[k, 0, :, mine], dev_z[k])
        z_wts[k] = remote(wts_out.at[k], wts.at[k], dev_z[k])

    def z_go(k, when=None):
        def start():
            @pl.when(above[k])
            def _():
                pl.semaphore_wait(up_sems.at[k], 1)

            z_rows[k].start()
            z_wts[k].start()

        start() if when is None else pl.when(when)(start)

    inner = jnp.abs(flipped(chip, ks[-1]) - chip) == 1

    def z_inner():
        z_go(ks[-1], inner)

    def z_outer():
        z_go(ks[-1], jnp.logical_not(inner))

    def rows_rx(k):
        relay_x(rows.at[k, 0], width, rg[k])

    def rows_ry(k):
        relay_y(rows.at[k, 0], width, rg[k])

    def rows_near(k):
        await_bytes(rows.at[k, 0, :, pl.ds(0, width)], rg[k]["late"])
        share(k, tp_x, width)
        share(k, tp_y, width)

    def rows_far(k):
        await_bytes(rows.at[k, 0, :, pl.ds(0, width)], rg[k]["far"])
        share(k, tp_d, width)

    def norm(k, p):
        if p == 1:
            await_bytes(rows.at[k, 1], sis[k])

        def body(r, carry):
            at = pl.ds(pl.multiple_of(r * 16, 16), 16)
            x = rows[k, p, at, :].astype(f32)
            ms = jnp.sum(x * x, axis=1, keepdims=True) / full
            inv = lax.rsqrt(ms + NORM_EPS)
            y = (x * inv * gain[...]).astype(bf16)
            normed[pl.ds(pl.multiple_of(p * capacity + r * 16, 16), 16), :] = y
            return carry

        lax.fori_loop(0, capacity // 16, body, 0)

    def up(k, n):
        if k == 0 and n == 0:
            loads[5].wait()
            loads[6].wait()
        half = hid_cols // 2
        at = slice(n * half, (n + 1) * half)
        x = normed[...]
        g = jnp.dot(x, wg[:, at], preferred_element_type=f32)
        u = jnp.dot(x, wu[:, at], preferred_element_type=f32)
        hid[k, :, cols(tp * 2 + n, half)] = (g / (1.0 + jnp.exp(-g)) * u).astype(bf16)

    senders = {"yl": send_yl, "xh": send_xh, "xl": send_xl, "yh": send_yh}

    def hs(k, name):
        if not hg[k]:
            hg[k]["late"] = hg[k]["far"] = recv_sem()
        senders[name](hid.at[k], hid_cols, hg[k])

    def hid_rx(k):
        relay_x(hid.at[k], hid_cols, hg[k])

    def hid_ry(k):
        relay_y(hid.at[k], hid_cols, hg[k])

    begun = []
    e_sends, z_back = {}, {}
    half_width = width // 2
    halves = [slice(h * half_width, (h + 1) * half_width) for h in (0, 1)]

    def down(k, h):
        if k not in begun:
            await_bytes(hid.at[k, :, pl.ds(0, 2 * hid_cols)], hg[k]["late"])
        if not begun:
            loads[7].wait()
        begun.append(k)

        def tile(n, carry):
            at = pl.ds(pl.multiple_of(h * half_width + n * 256, 256), 256)
            e = jnp.dot(hid[k], wd[:, at], preferred_element_type=f32).astype(bf16)
            e_own[k, :, at] = e[:capacity]
            e_send[k, :, at] = e[capacity:]
            return carry

        lax.fori_loop(0, half_width // 256, tile, 0)
        at = halves[h]
        e_sends[k, h] = go(e_send.at[k, :, at], e_recv.at[k, :, at], dev_s)

    def column(row):
        l128 = lax.broadcasted_iota(jnp.int32, (capacity, 128), 1)
        s128 = lax.broadcasted_iota(jnp.int32, (capacity, 128), 0)
        return jnp.sum(jnp.where(l128 == s128, row, 0.0), axis=1, keepdims=True)

    weights = {}

    def combine(k, h):
        if k not in weights:
            if k > 0:
                z_wts[k].wait_recv()
            w = wts[k]
            w_even, w_odd = column(w[0:1, :]), column(w[1:2, :])
            pick = core.astype(f32)
            weights[k] = (
                w_even * (1.0 - pick) + w_odd * pick, w_odd * (1.0 - pick) + w_even * pick
            )
        w_mine, w_other = weights[k]
        at = halves[h]
        e_sends[k, h].wait_recv()
        f = (e_own[k, :, at].astype(f32) * w_mine + e_recv[k, :, at].astype(f32) * w_other).astype(bf16)
        if k == 0:
            back[0, 0:capacity, at] = f
        else:
            feed_out[k, :, at] = f
            z_back[k, h] = go(feed_out.at[k, :, at], back.at[k, pl.ds(0, capacity), at], dev_z[k])

    def gather(k, h):
        if k > 0:
            z_back[k, h].wait_recv()
        at = halves[h]
        got = jnp.dot(pt[k], back[k, :, at], preferred_element_type=f32)
        if k == 0:
            out_ref[:, at] = (acc[:, at] + got).astype(bf16)
        else:
            acc[:, at] += got

    def clear():
        acc[...] = stream[...].astype(f32)
        for k in ks:
            back[k, capacity:, :] = jnp.zeros((128 - capacity, width), bf16)

    plan = [
        (rows_send, 0), (z_pick, 1), (z_go, 1), (z_pick, 2), (z_go, 2), (z_pick, 3), (rows_rx, 0),
        (rows_ry, 0), (rows_send, 1), (z_outer,), (rows_near, 0), (rows_ry, 1), (rows_far, 0), (rows_rx, 1),
        (norm, 0, 0), (z_inner,), (rows_send, 2), (norm, 0, 1), (up, 0, 0), (rows_near, 1), (up, 0, 1),
        (rows_rx, 2), (rows_far, 1), (rows_ry, 2), (rows_send, 3), (hs, 0, "xh"), (norm, 1, 0),
        (norm, 1, 1), (up, 1, 0), (rows_near, 2), (rows_far, 2), (up, 1, 1), (norm, 2, 0), (rows_ry, 3),
        (norm, 2, 1), (rows_rx, 3), (up, 2, 0), (hs, 2, "yl"), (up, 2, 1), (hs, 1, "yl"), (rows_near, 3),
        (hs, 2, "xh"), (hs, 2, "xl"), (rows_far, 3), (hs, 2, "yh"), (norm, 3, 0), (hid_rx, 2), (norm, 3, 1),
        (hid_ry, 2), (up, 3, 0), (hs, 3, "xl"), (hs, 3, "yl"), (up, 3, 1), (hs, 3, "xh"), (hs, 1, "xh"),
        (clear,), (hs, 3, "yh"), (hs, 1, "yh"), (down, 2, 1), (down, 2, 0), (hid_rx, 3), (combine, 2, 1),
        (hid_rx, 1), (hid_ry, 3), (hid_ry, 1), (hs, 0, "yl"), (hid_ry, 0), (combine, 2, 0), (hs, 1, "xl"),
        (down, 3, 0), (down, 3, 1), (hs, 0, "yh"), (combine, 3, 0), (hs, 0, "xl"), (down, 1, 0),
        (down, 1, 1), (hid_rx, 0), (combine, 1, 0), (gather, 2, 0), (combine, 1, 1), (combine, 3, 1),
        (down, 0, 1), (down, 0, 0), (gather, 1, 1), (gather, 2, 1), (gather, 3, 0), (combine, 0, 0),
        (gather, 1, 0), (combine, 0, 1), (gather, 0, 0), (gather, 3, 1), (gather, 0, 1),
    ]

    for step, *args in plan:
        name = step.__name__ + "".join("_" + str(a) for a in args)
        with jax.named_scope(name):
            step(*args)

    with jax.named_scope("drain"):
        for i, ref in enumerate((rows, hid)):
            pltpu.make_async_remote_copy(
                src_ref=ref, dst_ref=ref, send_sem=send_sems.at[i], recv_sem=recv_sems.at[0],
                device_id=dev_x, device_id_type=MESH,
            ).wait_send()
        for cp in sent:
            cp.wait_send()
        pl.when(sp < 2 * n_chips - 1)(edge.wait_send)
        if any(room) or count[0] != send_sems.shape[0] or count[1] != recv_sems.shape[0]:
            raise ValueError(f"semaphores {room} {count}")


def fused(
    b_gate,
    c_gate,
    h_in,
    docs,
    conv_taps,
    out_weight,
    residual_in,
    norm_gain,
    expert_pick,
    route_weight,
    w_gate,
    w_up,
    w_down,
):
    tok_rows, chans = h_in.shape
    width = residual_in.shape[1]
    full = w_gate.shape[1]
    hid_full = w_down.shape[1]
    n_sp = lax.axis_size("sp")
    n_chips = n_sp // 2
    capacity = 5 * tok_rows // (2 * n_sp)
    vmem = pl.BlockSpec(memory_space=pltpu.VMEM)
    hbm = pl.BlockSpec(memory_space=pltpu.HBM)
    bf16, f32 = jnp.bfloat16, jnp.float32
    return pl.pallas_call(
        functools.partial(fused_kernel, n_chips, capacity),
        out_shape=pltpu.VMEM((tok_rows, width), bf16),
        in_specs=[vmem] * 5 + [hbm] * 8,
        out_specs=vmem,
        scratch_shapes=[
            pltpu.VMEM(b_gate.shape, bf16),
            pltpu.VMEM(c_gate.shape, bf16),
            pltpu.VMEM(h_in.shape, bf16),
            pltpu.VMEM(residual_in.shape, bf16),
            pltpu.VMEM(out_weight.shape, bf16),
            pltpu.VMEM(w_gate.shape[1:], bf16),
            pltpu.VMEM(w_up.shape[1:], bf16),
            pltpu.VMEM(w_down.shape[1:], bf16),
            pltpu.VMEM((tok_rows + 8, chans), f32),
            pltpu.VMEM((tok_rows, out_weight.shape[0]), bf16),
            pltpu.VMEM((tok_rows, 128), f32),
            pltpu.VMEM((1, full), f32),
            pltpu.VMEM((tok_rows, width), bf16),
            pltpu.VMEM((tok_rows, width), f32),
            pltpu.VMEM((n_chips, tok_rows, 128), bf16),
            pltpu.VMEM((n_chips * capacity, tok_rows), bf16),
            pltpu.VMEM((n_chips, capacity, width), bf16),
            pltpu.VMEM((n_chips, 8, 128), f32),
            pltpu.VMEM((n_chips, 2, capacity, full), bf16),
            pltpu.VMEM((n_chips, 8, 128), f32),
            pltpu.VMEM((2 * capacity, full), bf16),
            pltpu.VMEM((n_chips, 2 * capacity, hid_full), bf16),
            pltpu.VMEM((n_chips, capacity, width), bf16),
            pltpu.VMEM((n_chips, capacity, width), bf16),
            pltpu.VMEM((n_chips, capacity, width), bf16),
            pltpu.VMEM((n_chips, capacity, width), bf16),
            pltpu.VMEM((n_chips, 128, width), bf16),
            pltpu.SemaphoreType.REGULAR((n_chips,)),
            pltpu.SemaphoreType.DMA((8,)),
            pltpu.SemaphoreType.DMA((19,)),
            pltpu.SemaphoreType.DMA((58,)),
        ],
        compiler_params=pltpu.CompilerParams(
            collective_id=0, has_side_effects=True, vmem_limit_bytes=66519040
        ),
    )(
        docs.reshape(1, -1),
        expert_pick.T,
        route_weight.T,
        conv_taps,
        norm_gain.reshape(-1, 128),
        b_gate,
        c_gate,
        h_in,
        residual_in,
        out_weight,
        w_gate,
        w_up,
        w_down,
    )


def pairs_fit(mesh):
    n_sp, n_tp = mesh.shape["sp"], mesh.shape["tp"]
    return n_sp == GROUPS * TOP_K and TOP_K == 2 and n_tp == 4


def solution(mesh):
    return jax.shard_map(
        fused if pairs_fit(mesh) else general,
        mesh=mesh,
        in_specs=(
            P("sp", "tp"),
            P("sp", "tp"),
            P("sp", "tp"),
            P(),
            P(),
            P(None, "tp"),
            P("sp", "tp"),
            P(),
            P("sp", None),
            P("sp", None),
            P("sp", None, "tp"),
            P("sp", None, "tp"),
            P("sp", None, "tp"),
        ),
        out_specs=P("sp", "tp"),
        check_vma=False,
    )
```

```python
import functools

import jax
import jax.numpy as jnp
from jax import lax
from jax.experimental import pallas as pl
from jax.experimental.pallas import tpu as pltpu
from jax.sharding import PartitionSpec as P

TOP_K = 2
GROUPS = 4
MESH = pl.DeviceIdType.MESH


NORM_EPS = 1e-06


def passed_along(value, axis, steps):
    count = lax.axis_size(axis)
    first, last = (max(0, -steps), min(count, count - steps))
    return lax.ppermute(value, axis, [(source, source + steps) for source in range(first, last)])


def general(
    b_gate,
    c_gate,
    h_in,
    docs,
    conv_taps,
    out_weight,
    residual_in,
    norm_gain,
    expert_pick,
    route_weight,
    w_gate,
    w_up,
    w_down,
):
    tok_rows, local_chans = h_in.shape
    width = residual_in.shape[1]
    full_dim = w_gate.shape[1]
    n_sp = lax.axis_size("sp")
    sp_index = lax.axis_index("sp")
    tp_index = lax.axis_index("tp")
    first_pos = sp_index * tok_rows
    product = (c_gate.astype(jnp.float32) * h_in.astype(jnp.float32)).astype(jnp.bfloat16)
    edge = passed_along(product[tok_rows - 2 :], "sp", 1)
    extended = jnp.concatenate([edge, product], axis=0).astype(jnp.float32)
    own_docs = lax.dynamic_slice_in_dim(docs, first_pos, tok_rows)
    padded_docs = jnp.concatenate([jnp.full((2,), -1, jnp.int32), docs], axis=0)
    near_docs = lax.dynamic_slice_in_dim(padded_docs, first_pos, tok_rows + 2)
    tap_weights = lax.dynamic_slice_in_dim(
        conv_taps, tp_index * local_chans, local_chans, 1
    ).astype(jnp.float32)
    conv_sum = tap_weights[0][None, :] * extended[2:]
    for step_back in (1, 2):
        same_doc = (near_docs[2 - step_back : 2 - step_back + tok_rows] == own_docs).astype(
            jnp.float32
        )[:, None]
        conv_sum = (
            conv_sum
            + tap_weights[step_back][None, :]
            * extended[2 - step_back : 2 - step_back + tok_rows]
            * same_doc
        )
    conv_out = (b_gate.astype(jnp.float32) * conv_sum).astype(jnp.bfloat16)
    projected = jnp.dot(
        lax.all_gather(conv_out, "tp", axis=1, tiled=True),
        out_weight,
        preferred_element_type=jnp.float32,
    )
    stream = (residual_in.astype(jnp.float32) + projected).astype(jnp.bfloat16)
    stream_f = stream.astype(jnp.float32)
    capacity = 5 * tok_rows // (2 * n_sp)
    assign_flat = expert_pick.reshape(-1)
    onehot = (assign_flat[:, None] == jnp.arange(n_sp, dtype=jnp.int32)[None, :]).astype(jnp.int32)
    slot_pos = jnp.sum((jnp.cumsum(onehot, axis=0) - onehot) * onehot, axis=1)
    kept_mask = slot_pos < capacity
    target = jnp.where(
        kept_mask, assign_flat * capacity + jnp.minimum(slot_pos, capacity - 1), n_sp * capacity
    )
    table = (
        jnp.full((n_sp * capacity + 1,), -1, jnp.int32)
        .at[target]
        .set(jnp.arange(assign_flat.shape[0], dtype=jnp.int32))[:-1]
    )
    filled = table >= 0
    source_rows = jnp.maximum(table, 0) // TOP_K
    gate_local = w_gate[0]
    up_local = w_up[0]
    slot_rows = n_sp * capacity
    squares = lax.psum(jnp.sum(stream_f * stream_f, axis=1), "tp")
    inverse = lax.rsqrt(squares / full_dim + NORM_EPS)[:, None]
    gain_cols = lax.dynamic_slice_in_dim(norm_gain, tp_index * width, width).astype(jnp.float32)
    normed = (stream_f * inverse * gain_cols[None, :]).astype(jnp.bfloat16)
    outgoing = jnp.where(filled[:, None], normed[source_rows], jnp.zeros((), normed.dtype)).reshape(
        n_sp, capacity, width
    )
    received = lax.all_to_all(outgoing, "sp", split_axis=0, concat_axis=0, tiled=True)
    shard_piece = lax.all_gather(received, "tp", axis=2, tiled=True)
    flat_piece = shard_piece.reshape(slot_rows, shard_piece.shape[2])
    gate_pre = jnp.dot(flat_piece, gate_local, preferred_element_type=jnp.float32)
    up_pre = jnp.dot(flat_piece, up_local, preferred_element_type=jnp.float32)
    hidden = (jax.nn.silu(gate_pre) * up_pre).astype(jnp.bfloat16)
    down_local = w_down[0]
    result = jnp.dot(
        lax.all_gather(hidden, "tp", axis=1, tiled=True),
        down_local,
        preferred_element_type=jnp.float32,
    ).astype(jnp.bfloat16)
    returned = lax.all_to_all(
        result.reshape(n_sp, capacity, width), "sp", split_axis=0, concat_axis=0, tiled=True
    ).reshape(n_sp * capacity, width)
    picked = jnp.where(
        kept_mask[:, None],
        returned[jnp.minimum(target, n_sp * capacity - 1)].astype(jnp.float32),
        0.0,
    )
    weighted = picked * route_weight.reshape(-1)[:, None]
    feed_out = jnp.sum(weighted.reshape(tok_rows, TOP_K, width), axis=1)
    return (stream_f + feed_out).astype(jnp.bfloat16)


def flipped(index, mask):
    bit = 1
    while bit <= mask:
        if mask & bit:
            index = index + bit * (1 - 2 * ((index // bit) % 2))
        bit *= 2
    return index


def fused_kernel(
    n_chips,
    capacity,
    docs_hbm,
    pick_hbm,
    rw_hbm,
    taps_hbm,
    gain_hbm,
    b_hbm,
    c_hbm,
    h_hbm,
    resid_hbm,
    ow_hbm,
    wg_hbm,
    wu_hbm,
    wd_hbm,
    out_ref,
    docs_ref,
    pick_ref,
    rw_ref,
    taps_ref,
    gain_ref,
    bb,
    cc,
    hh,
    resid,
    ow,
    wg,
    wu,
    wd,
    ext,
    cv,
    side,
    gain,
    stream,
    acc,
    pt,
    ptt,
    rows_out,
    wts_out,
    rows,
    wts,
    normed,
    hid,
    e_own,
    e_send,
    e_recv,
    feed_out,
    back,
    partial,
    up_sems,
    local_sems,
    send_sems,
    recv_sems,
):
    tok_rows, chans = hh.shape
    width = resid.shape[1]
    full = gain.shape[1]
    hid_cols = wg.shape[1]
    f32, bf16 = jnp.float32, jnp.bfloat16
    head = 16
    sp = lax.axis_index("sp")
    tp = lax.axis_index("tp")
    chip = sp // 2
    core = sp % 2
    tp_x = (tp // 2) * 2 + (1 - tp % 2)
    tp_y = (1 - tp // 2) * 2 + tp % 2
    tp_d = (1 - tp // 2) * 2 + (1 - tp % 2)
    dev_x = (sp, tp_x)
    dev_y = (sp, tp_y)
    dev_d = (sp, tp_d)
    dev_s = (chip * 2 + (1 - core), tp)
    ks = list(range(n_chips))
    dev_z = [(flipped(chip, k) * 2 + core, tp) for k in ks]

    barrier = pltpu.get_barrier_semaphore()
    plane = [dev_x, dev_y, dev_s]
    above = [flipped(chip, k) > chip for k in ks]
    edge_down = (core == 0) & (chip > 0)
    edge_up = (core == 1) & (chip < n_chips - 1)

    def signal(sem, dev):
        pl.semaphore_signal(sem, inc=1, device_id=dev, device_id_type=MESH)

    for dev in plane:
        signal(barrier, dev)
    for k in ks[1:]:
        pl.when(above[k])(functools.partial(signal, barrier, dev_z[k]))
    pl.when(edge_up)(functools.partial(signal, barrier, (sp + 1, tp)))
    pl.when(edge_down)(functools.partial(signal, barrier, (sp - 1, tp)))

    pairs = (
        (c_hbm, cc), (h_hbm, hh), (docs_hbm, docs_ref), (pick_hbm, pick_ref), (rw_hbm, rw_ref),
        (taps_hbm, taps_ref), (gain_hbm, gain_ref), (b_hbm, bb), (resid_hbm, resid),
        (ow_hbm, ow), (wg_hbm.at[0], wg), (wu_hbm.at[0], wu), (wd_hbm.at[0], wd),
    )
    loads = [pltpu.make_async_copy(s, d, local_sems.at[i]) for i, (s, d) in enumerate(pairs)]
    for cp in loads:
        cp.start()

    unit = capacity * width
    groups = [
        (rows, unit),
        (hid, unit),
        (rows.at[0, 0, :, pl.ds(0, 2 * width)], unit),
        (cv.at[pl.ds(head, tok_rows - head), pl.ds(0, 3 * chans)], (tok_rows - head) * chans),
        (cv.at[pl.ds(0, head), pl.ds(0, 3 * chans)], head * chans * 2),
        (wts_out.at[pl.ds(1, n_chips - 1)], 8 * 128 * 4),
    ]
    room = [ref.size * jnp.dtype(ref.dtype).itemsize for ref, _ in groups]
    count = [len(groups), 0]

    def recv_sem():
        count[1] += 1
        return recv_sems.at[count[1] - 1]

    def remote(s, d, dev, recv=None, own_send=False):
        size = s.size * jnp.dtype(s.dtype).itemsize
        if own_send:
            i = count[0]
            count[0] += 1
        else:
            i = [j for j, (_, step) in enumerate(groups) if room[j] >= size and size % step == 0][0]
            room[i] -= size
        cp = pltpu.make_async_remote_copy(
            src_ref=s, dst_ref=d, send_sem=send_sems.at[i],
            recv_sem=recv_sem() if recv is None else recv,
            device_id=dev, device_id_type=MESH,
        )
        return cp

    def go(s, d, dev, recv=None, own_send=False):
        cp = remote(s, d, dev, recv, own_send)
        cp.start()
        return cp

    def await_bytes(ref, recv):
        pltpu.make_async_remote_copy(
            src_ref=ref, dst_ref=ref, send_sem=send_sems.at[0], recv_sem=recv,
            device_id=dev_x, device_id_type=MESH,
        ).wait_recv()

    def cols(index, size):
        return pl.ds(pl.multiple_of(index * size, 128), size)

    for i in (2, 3, 4):
        loads[i].wait()
    sub8 = lax.broadcasted_iota(jnp.int32, (8, tok_rows), 0)
    own = docs_ref[:, cols(sp, tok_rows)]
    prev = docs_ref[:, pl.ds(pl.multiple_of(jnp.maximum(sp * tok_rows - 128, 0), 128), 128)]
    prev = jnp.where(sp > 0, prev, -1)
    near = jnp.broadcast_to(jnp.concatenate([prev, own], axis=1), (8, tok_rows + 128))
    own = jnp.broadcast_to(own, (8, tok_rows))
    same = [(pltpu.roll(near, lag, 1)[:, 128:] == own).astype(f32) for lag in (1, 2)]
    first = pick_ref[0:1, :]
    even = jnp.bitwise_and(first, 1) == 0
    w_a, w_b = rw_ref[0:1, :], rw_ref[1:2, :]
    table = [
        lax.shift_right_logical(first, 1).astype(f32),
        jnp.where(even, w_a, w_b),
        jnp.where(even, w_b, w_a),
    ]
    block = jnp.where(sub8 == 0, same[0], jnp.where(sub8 == 1, same[1], 0.0))
    for i, row in enumerate(table):
        block = jnp.where(sub8 == 2 + i, jnp.broadcast_to(row, (8, tok_rows)), block)
    block = jnp.concatenate([block, jnp.zeros((120, tok_rows), f32)], axis=0)
    side[...] = jnp.transpose(block)

    loads[0].wait()
    loads[1].wait()
    product = (cc[...].astype(f32) * hh[...].astype(f32)).astype(bf16)
    ext[8:, :] = product.astype(f32)
    with jax.named_scope("barrier"):
        pl.semaphore_wait(barrier, len(plane) + chip + (edge_down | edge_up).astype(jnp.int32))
    for k in ks[1:]:
        pl.when(flipped(chip, k) < chip)(functools.partial(signal, up_sems.at[k], dev_z[k]))
    signal(up_sems.at[0], dev_x)

    edge = remote(ext.at[pl.ds(tok_rows, 8)], ext.at[pl.ds(0, 8)], (sp + 1, tp), None, True)
    pl.when(sp < 2 * n_chips - 1)(edge.start)
    loads[7].wait()
    loads[5].wait()
    taps = taps_ref[:, cols(tp, chans)].astype(f32)

    def conv(lo, hi):
        total = taps[0:1, :] * ext[8 + lo : 8 + hi, :]
        for lag in (1, 2):
            part = ext[8 + lo - lag : 8 + hi - lag, :]
            total = total + taps[lag : lag + 1, :] * part * side[lo:hi, lag - 1 : lag]
        cv[lo:hi, cols(tp, chans)] = (bb[lo:hi, :].astype(f32) * total).astype(bf16)

    conv(head, tok_rows)

    def put(buf, at, dev, recv=None, own_send=False):
        part = buf.at[:, at]
        return go(part, part, dev, recv, own_send)

    def send_yl(buf, size, g):
        g["yl"] = put(buf, cols(tp * 2, size // 2), dev_y)

    def send_xh(buf, size, g):
        g["xh"] = put(buf, cols(tp * 2 + 1, size // 2), dev_x)

    def send_xl(buf, size, g):
        put(buf, cols(tp * 2, size // 2), dev_x, g["late"])

    def send_yh(buf, size, g):
        put(buf, cols(tp * 2 + 1, size // 2), dev_y, g["late"])

    def spread(buf, size, g):
        g["late"] = recv_sem()
        for send in (send_yl, send_xh, send_xl, send_yh):
            send(buf, size, g)

    def relay_x(buf, size, g):
        g["yl"].wait_recv()
        if "far" not in g:
            g["far"] = recv_sem()
        put(buf, cols(tp_y * 2, size // 2), dev_x, g["far"])

    def relay_y(buf, size, g):
        g["xh"].wait_recv()
        if "far" not in g:
            g["far"] = recv_sem()
        put(buf, cols(tp_x * 2 + 1, size // 2), dev_y, g["far"])

    def relay(buf, size, g):
        relay_x(buf, size, g)
        relay_y(buf, size, g)

    cg = {}
    body = cv.at[pl.ds(head, tok_rows - head)]
    spread(body, chans, cg)

    def proj(index):
        rows_ = pl.ds(pl.multiple_of(index * chans, 128), chans)
        return jnp.dot(cv[:, cols(index, chans)], ow[rows_, :], preferred_element_type=f32)


    lane = lax.broadcasted_iota(jnp.int32, (tok_rows, 128), 1)
    lane_f = lane.astype(f32)
    group = side[:, 2:3]
    onehot = (group == lane_f).astype(f32)
    earlier = (
        lax.broadcasted_iota(jnp.int32, (tok_rows, tok_rows), 1)
        < lax.broadcasted_iota(jnp.int32, (tok_rows, tok_rows), 0)
    ).astype(f32).astype(bf16)
    before = jnp.dot(earlier, onehot.astype(bf16), preferred_element_type=f32)
    slot = jnp.sum(before * onehot, axis=1, keepdims=True)

    def choose(k):
        here = flipped(chip, k).astype(f32)
        hit = jnp.where((group == here) & (slot == lane_f) & (lane < capacity), 1.0, 0.0)
        pt[k] = hit.astype(bf16)
        ptt[k * capacity : (k + 1) * capacity, :] = jnp.transpose(hit)[:capacity].astype(bf16)
        w0 = jnp.sum(hit * side[:, 3:4], axis=0, keepdims=True)
        w1 = jnp.sum(hit * side[:, 4:5], axis=0, keepdims=True)
        s8 = lax.broadcasted_iota(jnp.int32, (8, 128), 0)
        w0, w1 = jnp.broadcast_to(w0, (8, 128)), jnp.broadcast_to(w1, (8, 128))
        wts_out[k] = jnp.where(s8 == 0, w0, jnp.where(s8 == 1, w1, 0.0))

    choose(0)

    @pl.when(sp > 0)
    def _():
        with jax.named_scope("edge"):
            edge.wait_recv()

    @pl.when(sp == 0)
    def _():
        ext[0:8, :] = jnp.zeros((8, chans), f32)

    conv(0, head)
    top, top_sem = cv.at[pl.ds(0, head), cols(tp, chans)], recv_sem()
    go(top, top, dev_x, top_sem)
    go(top, top, dev_y, top_sem)
    pl.semaphore_wait(up_sems.at[0], 1)
    go(top, top, dev_d, top_sem)
    loads[8].wait()
    loads[9].wait()
    acc[...] = resid[...].astype(f32) + proj(tp)
    with jax.named_scope("crelay"):
        relay(body, chans, cg)
    for k in ks[1:]:
        choose(k)
    wts[0] = wts_out[0]
    loads[6].wait()
    gains = gain_ref[...].astype(f32)
    for j in range(full // 128):
        gain[:, j * 128 : (j + 1) * 128] = gains[j : j + 1, :]
    with jax.named_scope("top"):
        await_bytes(cv.at[pl.ds(0, head), pl.ds(0, 3 * chans)], top_sem)
    with jax.named_scope("cx"):
        await_bytes(body.at[:, pl.ds(0, chans)], cg["late"])
    acc[...] += proj(tp_x)
    acc[...] += proj(tp_y)
    with jax.named_scope("cd"):
        await_bytes(body.at[:, pl.ds(0, chans)], cg["far"])
    stream[...] = (acc[...] + proj(tp_d)).astype(bf16)

    mine = cols(tp, width)
    rg, hg = [{} for _ in ks], [{} for _ in ks]
    sis = [recv_sem() for _ in ks]
    z_rows, z_wts = {}, {}
    half_width = width // 2
    halves = [slice(h * half_width, (h + 1) * half_width) for h in (0, 1)]

    def share(k, index, size):
        at = cols(index, size)
        go(rows.at[k, 0, :, at], rows.at[k, 1, :, at], dev_s, sis[k])

    def select(k):
        at = slice(k * capacity, (k + 1) * capacity)
        return jnp.dot(ptt[at, :], stream[...], preferred_element_type=f32).astype(bf16)

    def rows_send(k, part):
        h = 1 if part == "hi" else 0
        if k > 0:
            z_rows[k, h].wait_recv()
        elif h == 1:
            rows[0, 0, :, mine] = select(0)
        buf = rows.at[k, 0]
        if "late" not in rg[k]:
            rg[k]["late"] = recv_sem()
        for send in (send_xh, send_yh) if h else (send_yl, send_xl):
            send(buf, width, rg[k])
        share(k, tp * 2 + h, half_width)

    def z_pick(k):
        rows_out[k] = select(k)
        for h in (1, 0):
            at = cols(tp * 2 + h, width // 2)
            src = rows_out.at[k, :, halves[h]]
            z_rows[k, h] = remote(src, rows.at[k, 0, :, at], dev_z[k])
        z_wts[k] = remote(wts_out.at[k], wts.at[k], dev_z[k])

    def z_go(k, when=None):
        def start():
            @pl.when(above[k])
            def _():
                pl.semaphore_wait(up_sems.at[k], 1)

            z_rows[k, 1].start()
            z_rows[k, 0].start()
            z_wts[k].start()

        start() if when is None else pl.when(when)(start)

    inner = jnp.abs(flipped(chip, ks[-1]) - chip) == 1

    def z_inner():
        z_go(ks[-1], inner)

    def z_outer():
        z_go(ks[-1], jnp.logical_not(inner))

    def rows_rx(k):
        relay_x(rows.at[k, 0], width, rg[k])

    def rows_ry(k):
        relay_y(rows.at[k, 0], width, rg[k])

    def rows_near(k):
        await_bytes(rows.at[k, 0, :, pl.ds(0, width)], rg[k]["late"])
        share(k, tp_x, width)
        share(k, tp_y, width)

    def rows_far(k):
        await_bytes(rows.at[k, 0, :, pl.ds(0, width)], rg[k]["far"])
        share(k, tp_d, width)

    def norm(k, p):
        if p == 1:
            await_bytes(rows.at[k, 1], sis[k])

        for r in range(capacity // 16):
            x = rows[k, p, r * 16 : (r + 1) * 16, :].astype(f32)
            ms = jnp.sum(x * x, axis=1, keepdims=True) / full
            inv = lax.rsqrt(ms + NORM_EPS)
            first = p * capacity + r * 16
            normed[first : first + 16, :] = (x * inv * gain[...]).astype(bf16)

    started = []

    def up(k, n):
        if not started:
            loads[10].wait()
            loads[11].wait()
        started.append(k)
        half = hid_cols // 2
        at = slice(n * half, (n + 1) * half)
        x = normed[...]
        g = jnp.dot(x, wg[:, at], preferred_element_type=f32)
        u = jnp.dot(x, wu[:, at], preferred_element_type=f32)
        hid[k, :, cols(tp * 2 + n, half)] = (g / (1.0 + jnp.exp(-g)) * u).astype(bf16)

    senders = {"yl": send_yl, "xh": send_xh, "xl": send_xl, "yh": send_yh}

    def hs(k, name):
        if not hg[k]:
            hg[k]["late"] = recv_sem()
            hg[k]["far"] = recv_sem() if k == 0 else hg[k]["late"]
        senders[name](hid.at[k], hid_cols, hg[k])

    def hid_rx(k):
        relay_x(hid.at[k], hid_cols, hg[k])

    def hid_ry(k):
        relay_y(hid.at[k], hid_cols, hg[k])

    begun = []
    e_sends, z_back = {}, {}

    def fetch_down():
        if not begun:
            loads[12].wait()
        begun.append(-1)

    def dot_down(k, index, at):
        rows_ = pl.ds(pl.multiple_of(index * hid_cols, 128), hid_cols)
        part = hid[k, :, cols(index, hid_cols)]
        return jnp.dot(part, wd[rows_, at], preferred_element_type=f32)

    def dpre(k):
        await_bytes(hid.at[k, :, pl.ds(0, hid_cols)], hg[k]["late"])
        fetch_down()

        def tile(n, carry):
            at = pl.ds(pl.multiple_of(n * 256, 256), 256)
            partial[:, at] = dot_down(k, tp, at) + dot_down(k, tp_x, at) + dot_down(k, tp_y, at)
            return carry

        lax.fori_loop(0, width // 256, tile, 0)

    def down(k, h):
        if k not in begun:
            if k == 0:
                await_bytes(hid.at[k, :, pl.ds(0, hid_cols)], hg[k]["far"])
            else:
                await_bytes(hid.at[k, :, pl.ds(0, 2 * hid_cols)], hg[k]["late"])
        fetch_down()
        begun.append(k)

        def tile(n, carry):
            at = pl.ds(pl.multiple_of(h * half_width + n * 256, 256), 256)
            if k == 0:
                e = partial[:, at] + dot_down(k, tp_d, at)
            else:
                e = jnp.dot(hid[k], wd[:, at], preferred_element_type=f32)
            e = e.astype(bf16)
            e_own[k, :, at] = e[:capacity]
            e_send[k, :, at] = e[capacity:]
            return carry

        lax.fori_loop(0, half_width // 256, tile, 0)
        at = halves[h]
        e_sends[k, h] = go(e_send.at[k, :, at], e_recv.at[k, :, at], dev_s)

    def column(row):
        l128 = lax.broadcasted_iota(jnp.int32, (capacity, 128), 1)
        s128 = lax.broadcasted_iota(jnp.int32, (capacity, 128), 0)
        return jnp.sum(jnp.where(l128 == s128, row, 0.0), axis=1, keepdims=True)

    weights = {}

    def combine(k, h):
        if k not in weights:
            if k > 0:
                z_wts[k].wait_recv()
            w = wts[k]
            w_even, w_odd = column(w[0:1, :]), column(w[1:2, :])
            pick = core.astype(f32)
            weights[k] = (
                w_even * (1.0 - pick) + w_odd * pick, w_odd * (1.0 - pick) + w_even * pick
            )
        w_mine, w_other = weights[k]
        at = halves[h]
        e_sends[k, h].wait_recv()
        f = (e_own[k, :, at].astype(f32) * w_mine + e_recv[k, :, at].astype(f32) * w_other).astype(bf16)
        if k == 0:
            back[0, 0:capacity, at] = f
        else:
            feed_out[k, :, at] = f
            z_back[k, h] = go(feed_out.at[k, :, at], back.at[k, pl.ds(0, capacity), at], dev_z[k])

    def gather(k, h):
        if k > 0:
            z_back[k, h].wait_recv()
        at = halves[h]
        got = jnp.dot(pt[k], back[k, :, at], preferred_element_type=f32)
        if k == 0:
            out_ref[:, at] = (acc[:, at] + got).astype(bf16)
        else:
            acc[:, at] += got

    def clear():
        acc[...] = stream[...].astype(f32)
        for k in ks:
            back[k, capacity:, :] = jnp.zeros((128 - capacity, width), bf16)

    plan = [
        (z_pick, 1), (z_go, 1), (rows_send, 0, "hi"), (z_pick, 3), (z_inner,), (z_pick, 2),
        (rows_send, 0, "lo"), (rows_send, 1, "hi"), (rows_send, 1, "lo"), (z_outer,), (z_go, 2), (clear,),
        (rows_send, 3, "hi"), (rows_send, 3, "lo"), (rows_ry, 1), (rows_rx, 1), (rows_rx, 0), (rows_ry, 3),
        (rows_near, 1), (rows_rx, 3), (rows_send, 2, "hi"), (rows_far, 1), (rows_send, 2, "lo"),
        (norm, 1, 0), (norm, 1, 1), (up, 1, 0), (rows_ry, 0), (rows_near, 0), (rows_near, 3), (rows_far, 3),
        (up, 1, 1), (hs, 1, "yh"), (norm, 3, 0), (hs, 1, "xl"), (norm, 3, 1), (up, 3, 0), (rows_rx, 2),
        (rows_ry, 2), (hs, 3, "yl"), (rows_far, 0), (hs, 1, "yl"), (up, 3, 1), (hs, 3, "xh"), (hs, 3, "xl"),
        (norm, 0, 0), (rows_near, 2), (norm, 0, 1), (hs, 3, "yh"), (up, 0, 0), (up, 0, 1), (rows_far, 2),
        (hs, 1, "xh"), (hid_rx, 3), (hid_ry, 3), (norm, 2, 0), (norm, 2, 1), (up, 2, 0), (hs, 2, "yl"),
        (up, 2, 1), (hs, 2, "xh"), (hid_rx, 1), (hid_ry, 1), (hs, 2, "xl"), (down, 3, 0), (hs, 2, "yh"),
        (hid_ry, 2), (hid_rx, 2), (combine, 3, 0), (hs, 0, "xh"), (hs, 0, "yl"), (down, 3, 1), (down, 1, 0),
        (down, 1, 1), (hs, 0, "xl"), (hs, 0, "yh"), (combine, 3, 1), (combine, 1, 0), (down, 2, 1),
        (combine, 2, 1), (hid_rx, 0), (combine, 1, 1), (hid_ry, 0), (down, 2, 0), (dpre, 0),
        (combine, 2, 0), (down, 0, 1), (gather, 3, 1), (down, 0, 0), (gather, 1, 0), (gather, 3, 0),
        (combine, 0, 1), (gather, 2, 1), (combine, 0, 0), (gather, 1, 1), (gather, 0, 1), (gather, 2, 0),
        (gather, 0, 0),
    ]

    for step, *args in plan:
        name = step.__name__ + "".join("_" + str(a) for a in args)
        with jax.named_scope(name):
            step(*args)

    with jax.named_scope("drain"):
        for i, (ref, _) in enumerate(groups):
            pltpu.make_async_remote_copy(
                src_ref=ref, dst_ref=ref, send_sem=send_sems.at[i], recv_sem=recv_sems.at[0],
                device_id=dev_x, device_id_type=MESH,
            ).wait_send()
        pl.when(sp < 2 * n_chips - 1)(edge.wait_send)
        if any(room) or count[0] != send_sems.shape[0] or count[1] != recv_sems.shape[0]:
            raise ValueError(f"semaphores {room} {count}")


def fused(
    b_gate,
    c_gate,
    h_in,
    docs,
    conv_taps,
    out_weight,
    residual_in,
    norm_gain,
    expert_pick,
    route_weight,
    w_gate,
    w_up,
    w_down,
):
    tok_rows, chans = h_in.shape
    width = residual_in.shape[1]
    full = w_gate.shape[1]
    hid_full = w_down.shape[1]
    n_sp = lax.axis_size("sp")
    n_chips = n_sp // 2
    capacity = 5 * tok_rows // (2 * n_sp)
    vmem = pl.BlockSpec(memory_space=pltpu.VMEM)
    hbm = pl.BlockSpec(memory_space=pltpu.HBM)
    bf16, f32 = jnp.bfloat16, jnp.float32
    return pl.pallas_call(
        functools.partial(fused_kernel, n_chips, capacity),
        out_shape=pltpu.VMEM((tok_rows, width), bf16),
        in_specs=[hbm] * 13,
        out_specs=vmem,
        scratch_shapes=[
            pltpu.VMEM((1, docs.shape[0]), jnp.int32),
            pltpu.VMEM((2, tok_rows), jnp.int32),
            pltpu.VMEM((2, tok_rows), f32),
            pltpu.VMEM(conv_taps.shape, bf16),
            pltpu.VMEM((full // 128, 128), bf16),
            pltpu.VMEM(b_gate.shape, bf16),
            pltpu.VMEM(c_gate.shape, bf16),
            pltpu.VMEM(h_in.shape, bf16),
            pltpu.VMEM(residual_in.shape, bf16),
            pltpu.VMEM(out_weight.shape, bf16),
            pltpu.VMEM(w_gate.shape[1:], bf16),
            pltpu.VMEM(w_up.shape[1:], bf16),
            pltpu.VMEM(w_down.shape[1:], bf16),
            pltpu.VMEM((tok_rows + 8, chans), f32),
            pltpu.VMEM((tok_rows, out_weight.shape[0]), bf16),
            pltpu.VMEM((tok_rows, 128), f32),
            pltpu.VMEM((1, full), f32),
            pltpu.VMEM((tok_rows, width), bf16),
            pltpu.VMEM((tok_rows, width), f32),
            pltpu.VMEM((n_chips, tok_rows, 128), bf16),
            pltpu.VMEM((n_chips * capacity, tok_rows), bf16),
            pltpu.VMEM((n_chips, capacity, width), bf16),
            pltpu.VMEM((n_chips, 8, 128), f32),
            pltpu.VMEM((n_chips, 2, capacity, full), bf16),
            pltpu.VMEM((n_chips, 8, 128), f32),
            pltpu.VMEM((2 * capacity, full), bf16),
            pltpu.VMEM((n_chips, 2 * capacity, hid_full), bf16),
            pltpu.VMEM((n_chips, capacity, width), bf16),
            pltpu.VMEM((n_chips, capacity, width), bf16),
            pltpu.VMEM((n_chips, capacity, width), bf16),
            pltpu.VMEM((n_chips, capacity, width), bf16),
            pltpu.VMEM((n_chips, 128, width), bf16),
            pltpu.VMEM((2 * capacity, width), f32),
            pltpu.SemaphoreType.REGULAR((n_chips,)),
            pltpu.SemaphoreType.DMA((13,)),
            pltpu.SemaphoreType.DMA((7,)),
            pltpu.SemaphoreType.DMA((62,)),
        ],
        compiler_params=pltpu.CompilerParams(
            collective_id=0, has_side_effects=True, vmem_limit_bytes=66519040
        ),
    )(
        docs.reshape(1, -1),
        expert_pick.T,
        route_weight.T,
        conv_taps,
        norm_gain.reshape(-1, 128),
        b_gate,
        c_gate,
        h_in,
        residual_in,
        out_weight,
        w_gate,
        w_up,
        w_down,
    )


def pairs_fit(mesh):
    n_sp, n_tp = mesh.shape["sp"], mesh.shape["tp"]
    return n_sp == GROUPS * TOP_K and TOP_K == 2 and n_tp == 4


def solution(mesh):
    return jax.shard_map(
        fused if pairs_fit(mesh) else general,
        mesh=mesh,
        in_specs=(
            P("sp", "tp"),
            P("sp", "tp"),
            P("sp", "tp"),
            P(),
            P(),
            P(None, "tp"),
            P("sp", "tp"),
            P(),
            P("sp", None),
            P("sp", None),
            P("sp", None, "tp"),
            P("sp", None, "tp"),
            P("sp", None, "tp"),
        ),
        out_specs=P("sp", "tp"),
        check_vma=False,
    )
```
